32 devices in a mesh: fs: 8 (over z, y), tp: 4 (over x, core).
Axes of the slice: x: 2, y: 2, z: 4, core: 2. Of those that a mesh axis runs over, the one named last changes fastest.
Arguments:
- up_pre: bfloat16 [6144, 4096], P('fs', 'tp'), may hold values from -6 to 6
- gate_value: bfloat16 [6144, 4096], P('fs', 'tp'), may hold values from -6 to 6
- out_cotangent: bfloat16 [6144, 2048], P('fs', 'tp'), may hold values from -8 to 8
- down_weight: bfloat16 [2048, 4096], P('fs', 'tp'), may hold values from -0.09375 to 0.09375
- conv_weight: float32 [3, 4096], P(None, 'tp'), may hold values from -3.5 to 3.5
- conv_bias: float32 [4096], P('tp'), may hold values from -3 to 3
Outputs:
- up_grad: bfloat16 [6144, 4096], P('fs', 'tp')
- gate_grad: bfloat16 [6144, 4096], P('fs', 'tp')
- weight_grad: float32 [2048, 4096], P('fs', 'tp')
- tap_grad: float32 [3, 4096], P(None, 'tp')
- bias_grad: float32 [4096], P('tp')
- unit_norms: float32 [4096], P('tp')
The draws below stay inside these ranges and needn't reach their ends.
All inputs are finite; a program needn't handle non-finite values.
Results may differ from the reference program's by a relative error of at most 0.0034.
Values may be sent and summed in bfloat16 or wider, within the bound.
No kernel may reach another device: no remote copies, remote signals or barrier semaphores. Data moves between devices by JAX's collectives and lax.ppermute only.
A program may use at most 64 MiB of HBM per device.

```python
import jax
import jax.numpy as jnp

D = 2048
FF = 4096
TAPS = 3
TOKENS = 6144


def raised(values, stream_key, source, target, shards_of, factor):
    owner, partner = [(jnp.arange(values.shape[position]) // (values.shape[position] // shards_of)).reshape([-1 if axis == position else 1 for axis in range(values.ndim)]) for position in (source, target)]
    chosen = jax.random.permutation(stream_key, shards_of)[partner]
    strong = (owner == chosen) | (owner == (partner + shards_of // 2) % shards_of)
    return jnp.where(strong, factor * values, values)


def level_of(key, dims, shards, least, largest):
    gain = 1.0
    for dim, shards_of in shards:
        heights = jax.random.uniform(jax.random.fold_in(jax.random.fold_in(key, 6), dim), (shards_of,), jnp.float32, least / len(shards), largest / len(shards))
        gain = gain * jnp.repeat(jnp.exp(heights), dims[dim] // shards_of).reshape((-1,) + (1,) * (len(dims) - 1 - dim))
    return gain


def noise(rng, shape, spread, reach, split=(), kind=jnp.bfloat16):
    drawn = spread * jax.random.normal(rng, shape, jnp.float32)
    if split:
        drawn = drawn * level_of(rng, shape, split, -0.22, 0.18)
    return jnp.clip(drawn, -reach, reach).astype(kind)


def heavy_noise(own_key, dims, spread, limit, pieces, heavy, held_as=jnp.bfloat16):
    drawn = spread * jax.random.normal(own_key, dims, jnp.float32)
    if pieces:
        drawn = drawn * level_of(own_key, dims, pieces, -0.22, 0.18)
    return jnp.clip(raised(drawn, jax.random.fold_in(own_key, 3), *heavy), -limit, limit).astype(held_as)


def setup_inputs(seed: int = 0) -> dict:
    seeds = jax.random.split(jax.random.key(seed), 7)
    up_pre = noise(seeds[0], (TOKENS, FF), 1.0, 6.0, ((0, 8), (1, 4)))
    gate_value = noise(seeds[1], (TOKENS, FF), 1.0, 6.0, ((0, 8), (1, 4)))
    out_cotangent = heavy_noise(seeds[2], (TOKENS, D), 1.0, 8.0, ((0, 8), (1, 4)), (0, 1, 8, 2.0))
    down_weight = noise(seeds[3], (D, FF), FF ** -0.5, 0.09375, ((0, 8), (1, 4)))
    conv_weight = noise(seeds[4], (TAPS, FF), TAPS ** -0.5, 3.5, ((1, 4),), jnp.float32)
    conv_bias = noise(seeds[5], (FF,), 0.5, 3.0, ((0, 4),), jnp.float32)
    return dict(up_pre=up_pre, gate_value=gate_value, out_cotangent=out_cotangent, down_weight=down_weight, conv_weight=conv_weight, conv_bias=conv_bias)


def reference(up_pre, gate_value, out_cotangent, down_weight, conv_weight, conv_bias):
    padded = jnp.pad(up_pre.astype(jnp.float32), ((TAPS - 1, 0), (0, 0)))
    conv_out = jnp.zeros((TOKENS, FF), jnp.float32) + conv_bias[None, :]
    for tap_index in range(TAPS):
        conv_out = conv_out + conv_weight[tap_index][None, :] * padded[tap_index:tap_index + TOKENS]
    sigmoid_val = jax.nn.sigmoid(conv_out)
    activated = conv_out * sigmoid_val
    gate_float = gate_value.astype(jnp.float32)
    hidden = (activated * gate_float).astype(jnp.bfloat16)
    hidden_grad = jnp.dot(out_cotangent, down_weight, preferred_element_type=jnp.float32)
    gate_grad = (hidden_grad * activated).astype(jnp.bfloat16)
    conv_grad = hidden_grad * gate_float * sigmoid_val * (1.0 + conv_out * (1.0 - sigmoid_val))
    after = jnp.pad(conv_grad, ((0, TAPS - 1), (0, 0)))
    up_grad = jnp.zeros((TOKENS, FF), jnp.float32)
    for tap_index in range(TAPS):
        lead = TAPS - 1 - tap_index
        up_grad = up_grad + conv_weight[tap_index][None, :] * after[lead:lead + TOKENS]
    tap_grad = jnp.stack([jnp.sum(conv_grad * padded[tap_index:tap_index + TOKENS], axis=0)
                          for tap_index in range(TAPS)])
    bias_grad = jnp.sum(conv_grad, axis=0)
    weight_grad = jnp.dot(out_cotangent.T, hidden, preferred_element_type=jnp.float32)
    unit_norms = jnp.sum(weight_grad * weight_grad, axis=0)
    return (up_grad.astype(jnp.bfloat16), gate_grad, weight_grad, tap_grad, bias_grad, unit_norms)
```

```python
import jax
import jax.numpy as jnp
from jax import lax
from jax.sharding import PartitionSpec as P


def flip(value, axis, mask):
    count = lax.axis_size(axis)
    return lax.ppermute(value, axis, [(i, i ^ mask) for i in range(count)])


def shift(value, axis, steps):
    count = lax.axis_size(axis)
    initial, last = (max(0, -steps), min(count, count - steps))
    return lax.ppermute(value, axis, [(source, source + steps) for source in range(initial, last)])


def reduce_all(value, axis):
    mask = 1
    while mask < lax.axis_size(axis):
        value = value + flip(value, axis, mask)
        mask *= 2
    return value


def per_device(up_pre, gate_value, out_cotangent, down_weight, conv_weight, conv_bias):
    tap_count = conv_weight.shape[0]
    tokens, units = up_pre.shape
    half = units // 2
    fs, tp = lax.axis_size("fs"), lax.axis_size("tp")
    me, col = lax.axis_index("fs"), lax.axis_index("tp")
    y = me % 2
    shard = down_weight.shape[0]
    width = out_cotangent.shape[1]
    depth = shard * fs

    w_mine = lax.dynamic_slice(down_weight, (0, y * half), (shard, half))
    w_send = lax.dynamic_slice(down_weight, (0, (1 - y) * half), (shard, half))
    w_pair = flip(w_send, "fs", 1)
    w_full = jnp.zeros((depth, half), down_weight.dtype)
    for mask in range(0, fs, 2):
        first = flip(w_mine, "fs", mask) if mask else w_mine
        second = flip(w_pair, "fs", mask) if mask else w_pair
        w_full = lax.dynamic_update_slice(w_full, first, ((me ^ mask) * shard, 0))
        w_full = lax.dynamic_update_slice(w_full, second, ((me ^ mask ^ 1) * shard, 0))

    cots = []
    for block in (out_cotangent, flip(out_cotangent, "fs", 1)):
        full = jnp.zeros((tokens, depth), block.dtype)
        for mask in range(0, tp, 2):
            piece = flip(block, "tp", mask) if mask else block
            full = lax.dynamic_update_slice(full, piece, (0, (col ^ mask) * width))
            full = lax.dynamic_update_slice(full, flip(piece, "tp", 1), (0, (col ^ mask ^ 1) * width))
        cots.append(full)
    cot_mine, cot_pair = cots

    before = shift(up_pre[tokens - (tap_count - 1) :], "fs", 1)
    padded = jnp.concatenate([before, up_pre], 0).astype(jnp.float32)
    conv_out = jnp.zeros(up_pre.shape, jnp.float32) + conv_bias[None, :]
    for tap in range(tap_count):
        conv_out = conv_out + conv_weight[tap][None, :] * padded[tap : tap + tokens]
    sigmoid_val = jax.nn.sigmoid(conv_out)
    activated = conv_out * sigmoid_val
    gate_float = gate_value.astype(jnp.float32)
    hidden = (activated * gate_float).astype(jnp.bfloat16)
    hid_mine = lax.dynamic_slice(hidden, (0, y * half), (tokens, half))
    hid_pair = flip(lax.dynamic_slice(hidden, (0, (1 - y) * half), (tokens, half)), "fs", 1)

    rows = 2 * shard
    total = None
    for mask in list(range(2, fs, 2)) + [0]:
        at = ((me ^ mask) // 2) * rows
        part = jnp.einsum(
            "td,tf->df",
            lax.dynamic_slice(cot_mine, (0, at), (tokens, rows)),
            hid_mine,
            preferred_element_type=jnp.float32,
        ) + jnp.einsum(
            "td,tf->df",
            lax.dynamic_slice(cot_pair, (0, at), (tokens, rows)),
            hid_pair,
            preferred_element_type=jnp.float32,
        )
        if mask:
            part = flip(part.astype(jnp.bfloat16), "fs", mask).astype(jnp.float32)
        total = part if total is None else total + part
    keep = lax.dynamic_slice(total, (y * shard, 0), (shard, half))
    give = lax.dynamic_slice(total, ((1 - y) * shard, 0), (shard, half)).astype(jnp.bfloat16)
    got = flip(give, "fs", 1).astype(jnp.float32)
    weight_grad = jnp.where(
        y == 0, jnp.concatenate([keep, got], 1), jnp.concatenate([got, keep], 1)
    )
    unit_norms = reduce_all(jnp.sum(weight_grad * weight_grad, axis=0), "fs")

    grad_mine = jnp.dot(cot_mine, w_full, preferred_element_type=jnp.float32)
    grad_send = jnp.dot(cot_pair, w_full, preferred_element_type=jnp.float32).astype(jnp.bfloat16)
    grad_got = flip(grad_send, "fs", 1).astype(jnp.float32)
    hidden_grad = jnp.where(
        y == 0,
        jnp.concatenate([grad_mine, grad_got], 1),
        jnp.concatenate([grad_got, grad_mine], 1),
    )
    gate_grad = (hidden_grad * activated).astype(jnp.bfloat16)
    conv_grad = hidden_grad * gate_float * sigmoid_val * (1.0 + conv_out * (1.0 - sigmoid_val))
    after = jnp.concatenate([conv_grad, shift(conv_grad[: tap_count - 1], "fs", -1)], 0)
    up_grad = jnp.zeros(up_pre.shape, jnp.float32)
    for tap in range(tap_count):
        lead = tap_count - 1 - tap
        up_grad = up_grad + conv_weight[tap][None, :] * after[lead : lead + tokens]
    sums = [jnp.sum(conv_grad * padded[tap : tap + tokens], axis=0) for tap in range(tap_count)]
    sums = reduce_all(jnp.stack(sums + [jnp.sum(conv_grad, axis=0)]), "fs")
    tap_grad, bias_grad = sums[:tap_count], sums[tap_count]
    return (up_grad.astype(jnp.bfloat16), gate_grad, weight_grad, tap_grad, bias_grad, unit_norms)


def solution(mesh):
    return jax.shard_map(
        per_device,
        mesh=mesh,
        in_specs=(
            P("fs", "tp"),
            P("fs", "tp"),
            P("fs", "tp"),
            P("fs", "tp"),
            P(None, "tp"),
            P("tp"),
        ),
        out_specs=(P("fs", "tp"), P("fs", "tp"), P("fs", "tp"), P(None, "tp"), P("tp"), P("tp")),
        check_vma=False,
    )
```

```python
import functools

import jax
import jax.numpy as jnp
from jax import lax
from jax.experimental import pallas as pl
from jax.experimental.pallas import tpu as pltpu
from jax.sharding import PartitionSpec as P


EDGE = 16
BF16, F32 = jnp.bfloat16, jnp.float32


def flip(value, axis, mask):
    count = lax.axis_size(axis)
    return lax.ppermute(value, axis, [(i, i ^ mask) for i in range(count)])


def shift(value, axis, steps):
    count = lax.axis_size(axis)
    initial, last = (max(0, -steps), min(count, count - steps))
    return lax.ppermute(value, axis, [(source, source + steps) for source in range(initial, last)])


def reduce_pairs(value, axis):
    parts = [value]
    for mask in range(2, lax.axis_size(axis), 2):
        parts.append(flip(value, axis, mask))
    return sum(parts)


def far_first(count):
    return list(range(4, count, 2)) + [2]


def conv_forward(up_ref, halo_ref, taps_ref, bias_ref):
    rows = up_ref.shape[0]
    full = jnp.concatenate([halo_ref[...], up_ref[...]], 0).astype(F32)
    count = taps_ref.shape[0]
    shifted = []
    for tap in range(count):
        lag = count - 1 - tap
        shifted.append((pltpu.roll(full, lag, 0) if lag else full)[EDGE : EDGE + rows])
    out = bias_ref[...]
    for tap in range(count):
        out = out + taps_ref[tap : tap + 1, :] * shifted[tap]
    return shifted, out


def hidden_kernel(y_ref, up_ref, halo_ref, gate_ref, taps_ref, bias_ref, send_ref, mine_ref, *, steps):
    _, out = conv_forward(up_ref, halo_ref, taps_ref, bias_ref)
    hidden = (out * jax.nn.sigmoid(out) * gate_ref[...].astype(F32)).astype(BF16)

    @pl.when(pl.program_id(0) < steps)
    def _():
        send_ref[...] = hidden

    @pl.when(pl.program_id(0) >= steps)
    def _():
        mine_ref[...] = hidden


def grads_kernel(
    y_ref, up_ref, halo_ref, gate_ref, taps_ref, bias_ref, own_ref, got_ref,
    gate_grad_ref, up_grad_ref, edge_ref, head_ref, sums_ref, *, steps,
):
    rows = up_ref.shape[0]
    count = taps_ref.shape[0]
    shifted, out = conv_forward(up_ref, halo_ref, taps_ref, bias_ref)
    sigmoid = jax.nn.sigmoid(out)
    hidden_grad = jnp.where(pl.program_id(0) < steps, own_ref[...], got_ref[...].astype(F32))
    gate_grad_ref[...] = (hidden_grad * (out * sigmoid)).astype(BF16)
    slope = sigmoid * (1.0 + out * (1.0 - sigmoid))
    grad = hidden_grad * gate_ref[...].astype(F32) * slope
    head_ref[...] = grad[: head_ref.shape[0]]
    width = grad.shape[1]
    padded = jnp.concatenate([grad, jnp.zeros((EDGE, width), F32)], 0)
    total = rows + EDGE
    up_grad = taps_ref[count - 1 : count, :] * grad
    for tap in range(count - 1):
        lead = count - 1 - tap
        up_grad = up_grad + taps_ref[tap : tap + 1, :] * pltpu.roll(padded, total - lead, 0)[:rows]
    up_grad_ref[...] = up_grad.astype(BF16)
    edge_ref[...] = up_grad[rows - EDGE :]
    sums = [jnp.sum(grad * part, 0, keepdims=True) for part in shifted]
    sums.append(jnp.sum(grad, 0, keepdims=True))
    fill = sums_ref.shape[0] - len(sums)
    sums_ref[...] = jnp.concatenate(sums + [jnp.zeros((fill, width), F32)], 0)


def column_specs(tokens, cols, steps, mine_first):
    def at(j, y_ref):
        own = (j < steps) if mine_first else (j >= steps)
        half = jnp.where(own, y_ref[0], 1 - y_ref[0])
        return half * steps + j % steps

    def spec(rows):
        return pl.BlockSpec((rows, cols), lambda j, y_ref: (0, at(j, y_ref)))

    first = pl.BlockSpec((tokens, cols), lambda j, y_ref: (0, jnp.minimum(j, steps - 1)))
    second = pl.BlockSpec((tokens, cols), lambda j, y_ref: (0, jnp.maximum(j - steps, 0)))
    return spec, first, second


def hidden_call(y, up_pre, halo, gate, taps, bias):
    tokens, units = up_pre.shape
    cols = min(256, units // 2)
    steps = units // 2 // cols
    spec, first, second = column_specs(tokens, cols, steps, False)
    half = jax.ShapeDtypeStruct((tokens, units // 2), BF16)
    return pl.pallas_call(
        functools.partial(hidden_kernel, steps=steps),
        out_shape=(half, half),
        grid_spec=pltpu.PrefetchScalarGridSpec(
            num_scalar_prefetch=1,
            grid=(2 * steps,),
            in_specs=[spec(tokens), spec(EDGE), spec(tokens), spec(taps.shape[0]), spec(1)],
            out_specs=(first, second),
        ),
        compiler_params=pltpu.CompilerParams(dimension_semantics=("arbitrary",)),
        cost_estimate=pl.CostEstimate(
            flops=20 * tokens * units, bytes_accessed=6 * tokens * units, transcendentals=0
        ),
    )(y, up_pre, halo, gate, taps, bias)


def grads_call(y, up_pre, halo, gate, taps, bias, own, got):
    tokens, units = up_pre.shape
    cols = min(256, units // 2)
    steps = units // 2 // cols
    spec, first, second = column_specs(tokens, cols, steps, True)
    count = 8 * ((taps.shape[0] + 8) // 8)
    return pl.pallas_call(
        functools.partial(grads_kernel, steps=steps),
        out_shape=(
            jax.ShapeDtypeStruct((tokens, units), BF16),
            jax.ShapeDtypeStruct((tokens, units), BF16),
            jax.ShapeDtypeStruct((EDGE, units), F32),
            jax.ShapeDtypeStruct((8, units), F32),
            jax.ShapeDtypeStruct((count, units), F32),
        ),
        grid_spec=pltpu.PrefetchScalarGridSpec(
            num_scalar_prefetch=1,
            grid=(2 * steps,),
            in_specs=[
                spec(tokens), spec(EDGE), spec(tokens), spec(taps.shape[0]), spec(1), first, second,
            ],
            out_specs=(spec(tokens), spec(tokens), spec(EDGE), spec(8), spec(count)),
        ),
        compiler_params=pltpu.CompilerParams(dimension_semantics=("arbitrary",)),
        cost_estimate=pl.CostEstimate(
            flops=50 * tokens * units, bytes_accessed=11 * tokens * units, transcendentals=0
        ),
    )(y, up_pre, halo, gate, taps, bias, own, got)


def paired(up_pre, gate_value, out_cotangent, down_weight, conv_weight, conv_bias):
    tap_count = conv_weight.shape[0]
    tokens, units = up_pre.shape
    half = units // 2
    fs, tp = lax.axis_size("fs"), lax.axis_size("tp")
    me, col = lax.axis_index("fs"), lax.axis_index("tp")
    y = me % 2
    shard = down_weight.shape[0]
    width = out_cotangent.shape[1]
    depth = shard * fs
    which = y.reshape(1).astype(jnp.int32)
    bias = conv_bias[None, :]

    w_mine = lax.dynamic_slice(down_weight, (0, y * half), (shard, half))
    w_send = lax.dynamic_slice(down_weight, (0, (1 - y) * half), (shard, half))
    w_pair = flip(w_send, "fs", 1)
    w_full = jnp.zeros((depth, half), down_weight.dtype)
    for mask in far_first(fs) + [0]:
        first = flip(w_mine, "fs", mask) if mask else w_mine
        second = flip(w_pair, "fs", mask) if mask else w_pair
        w_full = lax.dynamic_update_slice(w_full, first, ((me ^ mask) * shard, 0))
        w_full = lax.dynamic_update_slice(w_full, second, ((me ^ mask ^ 1) * shard, 0))

    cots = []
    for block in (out_cotangent, flip(out_cotangent, "fs", 1)):
        full = jnp.zeros((tokens, depth), block.dtype)
        for mask in range(0, tp, 2):
            piece = flip(block, "tp", mask) if mask else block
            other = flip(piece, "tp", 1)
            full = lax.dynamic_update_slice(full, piece, (0, (col ^ mask) * width))
            full = lax.dynamic_update_slice(full, other, (0, (col ^ mask ^ 1) * width))
        cots.append(full)
    cot_mine, cot_pair = cots

    halo = shift(up_pre[tokens - EDGE :], "fs", 1)
    hid_send, hid_mine = hidden_call(which, up_pre, halo, gate_value, conv_weight, bias)
    hid_pair = flip(hid_send, "fs", 1)

    rows = 2 * shard
    total = None
    for mask in far_first(fs) + [0]:
        at = ((me ^ mask) // 2) * rows
        part = jnp.einsum(
            "td,tf->df",
            lax.dynamic_slice(cot_mine, (0, at), (tokens, rows)),
            hid_mine,
            preferred_element_type=F32,
        ) + jnp.einsum(
            "td,tf->df",
            lax.dynamic_slice(cot_pair, (0, at), (tokens, rows)),
            hid_pair,
            preferred_element_type=F32,
        )
        if mask:
            part = flip(part.astype(BF16), "fs", mask).astype(F32)
        total = part if total is None else total + part
    keep = lax.dynamic_slice(total, (y * shard, 0), (shard, half))
    give = lax.dynamic_slice(total, ((1 - y) * shard, 0), (shard, half)).astype(BF16)
    got = flip(give, "fs", 1).astype(F32)
    weight_grad = jnp.where(
        y == 0, jnp.concatenate([keep, got], 1), jnp.concatenate([got, keep], 1)
    )

    grad_send = jnp.dot(cot_pair, w_full, preferred_element_type=F32).astype(BF16)
    grad_got = flip(grad_send, "fs", 1)
    grad_mine = jnp.dot(cot_mine, w_full, preferred_element_type=F32)
    gate_grad, up_grad, edge, head, sums = grads_call(
        which, up_pre, halo, gate_value, conv_weight, bias, grad_mine, grad_got
    )
    after = shift(head, "fs", -1)
    for tap in range(tap_count - 1):
        lead = tap_count - 1 - tap
        edge = edge.at[EDGE - lead :].add(conv_weight[tap][None, :] * after[:lead])
    up_grad = lax.dynamic_update_slice(up_grad, edge.astype(BF16), (tokens - EDGE, 0))

    sums = sums[: tap_count + 1]
    sums = (sums + flip(sums, "fs", 1)).reshape(-1)
    sums = jnp.concatenate([sums, jnp.sum(total * total, axis=0)])
    sums = reduce_pairs(sums, "fs")
    norm_mine = sums[-half:]
    sums = sums[:-half].reshape(tap_count + 1, units)
    norm_pair = flip(norm_mine, "fs", 1)
    unit_norms = jnp.where(
        y == 0, jnp.concatenate([norm_mine, norm_pair]), jnp.concatenate([norm_pair, norm_mine])
    )
    return (up_grad, gate_grad, weight_grad, sums[:tap_count], sums[tap_count], unit_norms)


def gathered(up_pre, gate_value, out_cotangent, down_weight, conv_weight, conv_bias):
    tap_count = conv_weight.shape[0]
    tokens = up_pre.shape[0]
    before = shift(up_pre[tokens - (tap_count - 1) :], "fs", 1)
    padded = jnp.concatenate([before, up_pre], 0).astype(F32)
    conv_out = jnp.zeros(up_pre.shape, F32) + conv_bias[None, :]
    for tap in range(tap_count):
        conv_out = conv_out + conv_weight[tap][None, :] * padded[tap : tap + tokens]
    sigmoid_val = jax.nn.sigmoid(conv_out)
    activated = conv_out * sigmoid_val
    gate_float = gate_value.astype(F32)
    hidden = (activated * gate_float).astype(BF16)
    full_cot = lax.all_gather(out_cotangent, "tp", axis=1, tiled=True)
    full_weight = lax.all_gather(down_weight, "fs", axis=0, tiled=True)
    hidden_grad = jnp.dot(full_cot, full_weight, preferred_element_type=F32)
    gate_grad = (hidden_grad * activated).astype(BF16)
    conv_grad = hidden_grad * gate_float * sigmoid_val * (1.0 + conv_out * (1.0 - sigmoid_val))
    after = jnp.concatenate([conv_grad, shift(conv_grad[: tap_count - 1], "fs", -1)], 0)
    up_grad = jnp.zeros(up_pre.shape, F32)
    for tap in range(tap_count):
        lead = tap_count - 1 - tap
        up_grad = up_grad + conv_weight[tap][None, :] * after[lead : lead + tokens]
    sums = [jnp.sum(conv_grad * padded[tap : tap + tokens], axis=0) for tap in range(tap_count)]
    sums = lax.psum(jnp.stack(sums + [jnp.sum(conv_grad, axis=0)]), "fs")
    partial_value = jnp.einsum("td,tf->df", full_cot, hidden, preferred_element_type=F32)
    weight_grad = lax.psum_scatter(partial_value, "fs", scatter_dimension=0, tiled=True)
    unit_norms = lax.psum(jnp.sum(weight_grad * weight_grad, axis=0), "fs")
    return (up_grad.astype(BF16), gate_grad, weight_grad, sums[:tap_count], sums[tap_count], unit_norms)


def solution(mesh):
    fs, tp = mesh.shape["fs"], mesh.shape["tp"]
    short = fs in (4, 8) and tp in (2, 4)

    def step(*args):
        return (paired if short else gathered)(*args)

    return jax.shard_map(
        step,
        mesh=mesh,
        in_specs=(
            P("fs", "tp"),
            P("fs", "tp"),
            P("fs", "tp"),
            P("fs", "tp"),
            P(None, "tp"),
            P("tp"),
        ),
        out_specs=(P("fs", "tp"), P("fs", "tp"), P("fs", "tp"), P(None, "tp"), P("tp"), P("tp")),
        check_vma=False,
    )
```

```python
import functools

import jax
import jax.numpy as jnp
from jax import lax
from jax.experimental import pallas as pl
from jax.experimental.pallas import tpu as pltpu
from jax.sharding import PartitionSpec as P


GRANT = 20 * 2**20
WIDE = 52 * 2**20
EDGE = 16
BF16, F32 = jnp.bfloat16, jnp.float32


def flip(value, axis, mask):
    count = lax.axis_size(axis)
    return lax.ppermute(value, axis, [(i, i ^ mask) for i in range(count)])


def shift(value, axis, steps):
    count = lax.axis_size(axis)
    initial, last = (max(0, -steps), min(count, count - steps))
    return lax.ppermute(value, axis, [(source, source + steps) for source in range(initial, last)])


def grant(size=GRANT):
    return pltpu.CompilerParams(vmem_limit_bytes=size)


def conv_forward(up_ref, halo_ref, taps_ref, bias_ref):
    rows = up_ref.shape[0]
    full = jnp.concatenate([halo_ref[...], up_ref[...]], 0).astype(F32)
    count = taps_ref.shape[0]
    shifted = []
    for tap in range(count):
        lag = count - 1 - tap
        shifted.append((pltpu.roll(full, lag, 0) if lag else full)[EDGE : EDGE + rows])
    out = bias_ref[...]
    for tap in range(count):
        out = out + taps_ref[tap : tap + 1, :] * shifted[tap]
    return shifted, out


def hidden_kernel(y_ref, up_ref, halo_ref, gate_ref, taps_ref, bias_ref, send_ref, mine_ref, *, steps):
    _, out = conv_forward(up_ref, halo_ref, taps_ref, bias_ref)
    hidden = (out * jax.nn.sigmoid(out) * gate_ref[...].astype(F32)).astype(BF16).T

    @pl.when(pl.program_id(0) < steps)
    def _():
        send_ref[...] = hidden

    @pl.when(pl.program_id(0) >= steps)
    def _():
        mine_ref[...] = hidden


def grads_kernel(
    y_ref, up_ref, halo_ref, gate_ref, taps_ref, bias_ref, own_ref, got_ref,
    gate_grad_ref, up_grad_ref, edge_ref, head_ref, sums_ref, *, steps,
):
    rows = up_ref.shape[0]
    count = taps_ref.shape[0]
    shifted, out = conv_forward(up_ref, halo_ref, taps_ref, bias_ref)
    sigmoid = jax.nn.sigmoid(out)
    hidden_grad = jnp.where(pl.program_id(0) < steps, own_ref[...], got_ref[...].astype(F32))
    gate_grad_ref[...] = (hidden_grad * (out * sigmoid)).astype(BF16)
    slope = sigmoid * (1.0 + out * (1.0 - sigmoid))
    grad = hidden_grad * gate_ref[...].astype(F32) * slope
    head_ref[...] = grad[: head_ref.shape[0]]
    width = grad.shape[1]
    padded = jnp.concatenate([grad, jnp.zeros((EDGE, width), F32)], 0)
    total = rows + EDGE
    up_grad = taps_ref[count - 1 : count, :] * grad
    for tap in range(count - 1):
        lead = count - 1 - tap
        up_grad = up_grad + taps_ref[tap : tap + 1, :] * pltpu.roll(padded, total - lead, 0)[:rows]
    up_grad_ref[...] = up_grad.astype(BF16)
    edge_ref[...] = up_grad[rows - EDGE :]
    sums = [jnp.sum(grad * part, 0, keepdims=True) for part in shifted]
    sums.append(jnp.sum(grad, 0, keepdims=True))
    fill = sums_ref.shape[0] - len(sums)
    sums_ref[...] = jnp.concatenate(sums + [jnp.zeros((fill, width), F32)], 0)


def column_specs(tokens, cols, steps, mine_first):
    def at(j, y_ref):
        own = (j < steps) if mine_first else (j >= steps)
        y = y_ref[0] % 2
        half = jnp.where(own, y, 1 - y)
        return half * steps + j % steps

    def spec(rows):
        return pl.BlockSpec((rows, cols), lambda j, y_ref: (0, at(j, y_ref)))

    first = pl.BlockSpec((tokens, cols), lambda j, y_ref: (0, jnp.minimum(j, steps - 1)))
    second = pl.BlockSpec((tokens, cols), lambda j, y_ref: (0, jnp.maximum(j - steps, 0)))
    return spec, first, second


def hidden_call(y, up_pre, halo, gate, taps, bias):
    tokens, units = up_pre.shape
    cols = min(256, units // 2)
    steps = units // 2 // cols
    spec, _, _ = column_specs(tokens, cols, steps, False)
    first = pl.BlockSpec((cols, tokens), lambda j, y_ref: (jnp.minimum(j, steps - 1), 0))
    second = pl.BlockSpec((cols, tokens), lambda j, y_ref: (jnp.maximum(j - steps, 0), 0))
    half = jax.ShapeDtypeStruct((units // 2, tokens), BF16)
    return pl.pallas_call(
        functools.partial(hidden_kernel, steps=steps),
        out_shape=(half, half),
        grid_spec=pltpu.PrefetchScalarGridSpec(
            num_scalar_prefetch=1,
            grid=(2 * steps,),
            in_specs=[spec(tokens), spec(EDGE), spec(tokens), spec(taps.shape[0]), spec(1)],
            out_specs=(first, second),
        ),
        compiler_params=grant(WIDE),
        cost_estimate=pl.CostEstimate(
            flops=20 * tokens * units, bytes_accessed=6 * tokens * units, transcendentals=0
        ),
    )(y, up_pre, halo, gate, taps, bias)


def grads_call(y, up_pre, halo, gate, taps, bias, own, got):
    tokens, units = up_pre.shape
    cols = min(256, units // 2)
    steps = units // 2 // cols
    spec, first, second = column_specs(tokens, cols, steps, True)
    count = 8 * ((taps.shape[0] + 8) // 8)
    return pl.pallas_call(
        functools.partial(grads_kernel, steps=steps),
        out_shape=(
            jax.ShapeDtypeStruct((tokens, units), BF16),
            jax.ShapeDtypeStruct((tokens, units), BF16),
            jax.ShapeDtypeStruct((EDGE, units), F32),
            jax.ShapeDtypeStruct((8, units), F32),
            jax.ShapeDtypeStruct((count, units), F32),
        ),
        grid_spec=pltpu.PrefetchScalarGridSpec(
            num_scalar_prefetch=1,
            grid=(2 * steps,),
            in_specs=[
                spec(tokens), spec(EDGE), spec(tokens), spec(taps.shape[0]), spec(1), first, second,
            ],
            out_specs=(spec(tokens), spec(tokens), spec(EDGE), spec(8), spec(count)),
        ),
        compiler_params=grant(),
        cost_estimate=pl.CostEstimate(
            flops=50 * tokens * units, bytes_accessed=11 * tokens * units, transcendentals=0
        ),
    )(y, up_pre, halo, gate, taps, bias, own, got)


def parts_kernel(ids_ref, *refs, masks, groups):
    count = sum(len(group) for group in groups)
    hid_mine_ref, hid_pair_ref = refs[count : count + 2]
    out_refs, block_ref = refs[count + 2 : -1], refs[-1]
    rows = block_ref.shape[1]
    per = refs[0].shape[1] // rows
    hidden = jnp.concatenate([hid_mine_ref[...], hid_pair_ref[...]], 1)
    for step, out_ref in enumerate(out_refs):
        block = ids_ref[0] ^ masks[step]
        begin = pl.multiple_of(lax.rem(block, per) * rows, rows)
        for piece in range(len(groups[0])):

            @pl.when(lax.div(block, per) ^ ids_ref[1] == piece)
            def _(piece=piece, begin=begin):
                top = 0
                for group in groups:
                    ref = refs[group[piece]]
                    tokens = ref.shape[0]
                    block_ref[top : top + tokens] = ref[:, pl.ds(begin, rows)]
                    top += tokens

        part = jnp.dot(hidden, block_ref[...], preferred_element_type=F32)
        out_ref[...] = part.astype(out_ref.dtype)


def in_vmem(count):
    return (pl.BlockSpec(memory_space=pltpu.VMEM),) * count


def parts_call(ids, masks, types, rows, cots, hid_mine, hid_pair):
    half, tokens = hid_mine.shape
    count, pieces = len(types), len(cots[0])
    groups = tuple(tuple(range(i * pieces, (i + 1) * pieces)) for i in range(len(cots)))
    return pl.pallas_call(
        functools.partial(parts_kernel, masks=tuple(masks), groups=groups),
        out_shape=tuple(jax.ShapeDtypeStruct((half, rows), kind) for kind in types),
        in_specs=(pl.BlockSpec(memory_space=pltpu.SMEM), *in_vmem(len(cots) * pieces + 2)),
        out_specs=in_vmem(count),
        scratch_shapes=[pltpu.VMEM((2 * tokens, rows), BF16)],
        compiler_params=grant(),
        cost_estimate=pl.CostEstimate(
            flops=4 * tokens * rows * half * count,
            bytes_accessed=4 * tokens * (half + rows * count),
            transcendentals=0,
        ),
    )(ids, *(piece for cot in cots for piece in cot), hid_mine, hid_pair)


def product_kernel(ids_ref, *refs, masks, groups):
    weights, (out_ref, full_ref) = refs[: len(masks)], refs[-2:]
    rows = weights[0].shape[0]
    per = refs[groups[0][0]].shape[1] // rows
    for mask, weight_ref in zip(masks, weights):
        block = ids_ref[0] ^ mask
        at = (lax.div(block, per) ^ ids_ref[1]) * per + lax.rem(block, per)
        full_ref[pl.ds(pl.multiple_of(at * rows, rows), rows), :] = weight_ref[...]
    top = 0
    for group in groups:
        cot = jnp.concatenate([refs[index][...] for index in group], 1)
        part = jnp.dot(cot, full_ref[...], preferred_element_type=F32)
        out_ref[top : top + cot.shape[0]] = part.astype(out_ref.dtype)
        top += cot.shape[0]


def product_call(ids, masks, weights, cots, kind):
    tokens = sum(cot[0].shape[0] for cot in cots)
    rows, half = weights[0].shape
    depth, pieces, start = rows * len(weights), len(cots[0]), len(weights)
    groups = tuple(
        tuple(range(start + i * pieces, start + (i + 1) * pieces)) for i in range(len(cots))
    )
    return pl.pallas_call(
        functools.partial(product_kernel, masks=tuple(masks), groups=groups),
        out_shape=jax.ShapeDtypeStruct((tokens, half), kind),
        in_specs=(
            pl.BlockSpec(memory_space=pltpu.SMEM), *in_vmem(len(weights) + len(cots) * pieces),
        ),
        out_specs=pl.BlockSpec(memory_space=pltpu.VMEM),
        scratch_shapes=[pltpu.VMEM((depth, half), BF16)],
        compiler_params=grant(),
        cost_estimate=pl.CostEstimate(
            flops=2 * tokens * depth * half,
            bytes_accessed=2 * (tokens + half) * depth,
            transcendentals=0,
        ),
    )(ids, *weights, *(piece for cot in cots for piece in cot))


def settle_kernel(own_ref, far_ref, near_ref, out_ref, norm_ref):
    total = own_ref[...] + far_ref[...].astype(F32) + near_ref[...].astype(F32)
    total = total.T
    out_ref[...] = total.astype(out_ref.dtype)
    norm_ref[...] = jnp.sum(total * total, 0, keepdims=True)


def settle_call(own, far, near, kind):
    half, rows = own.shape
    return pl.pallas_call(
        settle_kernel,
        out_shape=(
            jax.ShapeDtypeStruct((rows, half), kind),
            jax.ShapeDtypeStruct((1, half), F32),
        ),
        in_specs=in_vmem(3),
        out_specs=in_vmem(2),
        compiler_params=grant(),
        cost_estimate=pl.CostEstimate(
            flops=6 * half * rows, bytes_accessed=12 * half * rows, transcendentals=0
        ),
    )(own, far, near)


def join_kernel(ids_ref, kept_ref, got_ref, out_ref):
    kept, got = kept_ref[...], got_ref[...].astype(F32)
    first = ids_ref[0] % 2 == 0
    half = kept.shape[1]
    out_ref[:, :half] = jnp.where(first, kept, got)
    out_ref[:, half:] = jnp.where(first, got, kept)


def join_call(ids, kept, got):
    rows, half = kept.shape
    return pl.pallas_call(
        join_kernel,
        out_shape=jax.ShapeDtypeStruct((rows, 2 * half), F32),
        in_specs=(pl.BlockSpec(memory_space=pltpu.SMEM), *in_vmem(2)),
        out_specs=pl.BlockSpec(memory_space=pltpu.VMEM),
        compiler_params=grant(),
        cost_estimate=pl.CostEstimate(
            flops=2 * half * rows, bytes_accessed=14 * half * rows, transcendentals=0
        ),
    )(ids, kept, got)


def finish_kernel(y_ref, v0_ref, v2_ref, v1_ref, v3_ref, tap_ref, bias_ref, norm_ref):
    mine = v0_ref[...] + v2_ref[...]
    pair = v1_ref[...] + v3_ref[...]
    count = tap_ref.shape[0]
    half = norm_ref.shape[1] // 2
    both = mine + pair
    tap_ref[...] = both[:count]
    bias_ref[...] = both[count : count + 1]
    a, b = mine[count + 1 : count + 2, :half], pair[count + 1 : count + 2, :half]
    norm_ref[...] = jnp.where(
        y_ref[0] % 2 == 0, jnp.concatenate([a, b], 1), jnp.concatenate([b, a], 1)
    )


def finish_call(y, values, count):
    units = values[0].shape[1]
    row = jax.ShapeDtypeStruct((1, units), F32)
    return pl.pallas_call(
        finish_kernel,
        out_shape=(jax.ShapeDtypeStruct((count, units), F32), row, row),
        in_specs=[pl.BlockSpec(memory_space=pltpu.SMEM)]
        + [pl.BlockSpec(memory_space=pltpu.VMEM)] * len(values),
        out_specs=(pl.BlockSpec(memory_space=pltpu.VMEM),) * 3,
        compiler_params=grant(),
    )(y, *values)


def paired(up_pre, gate_value, out_cotangent, down_weight, conv_weight, conv_bias):
    tap_count = conv_weight.shape[0]
    tokens, units = up_pre.shape
    half = units // 2
    me, col = lax.axis_index("fs"), lax.axis_index("tp")
    shard = down_weight.shape[0]
    y = me % 2
    ids = lax.optimization_barrier(jnp.stack([me, col]).astype(jnp.int32))
    bias = conv_bias[None, :]

    def features(block):
        over = flip(block, "tp", 2)
        return block, flip(block, "tp", 1), over, flip(over, "tp", 1)

    cot_mine = features(out_cotangent)
    cot_pair = features(flip(out_cotangent, "fs", 1))

    w_mine = lax.dynamic_slice(down_weight, (0, y * half), (shard, half))
    w_send = lax.dynamic_slice(down_weight, (0, (1 - y) * half), (shard, half))
    weights, weight_masks = [], []
    for block, odd in ((w_mine, 0), (flip(w_send, "fs", 1), 1)):
        far = flip(block, "fs", 4)
        weights += [block, flip(block, "fs", 2), far, flip(far, "fs", 2)]
        weight_masks += [mask ^ odd for mask in (0, 2, 4, 6)]

    halo = shift(up_pre[tokens - EDGE :], "fs", 1)
    hid_send, hid_mine = hidden_call(ids, up_pre, halo, gate_value, conv_weight, bias)
    hid_pair = flip(hid_send, "fs", 1)

    operands = (shard, (cot_mine, cot_pair), hid_mine, hid_pair)
    masks = [mask ^ odd for mask in (6, 4, 2, 0) for odd in (1, 0)]
    p6 = parts_call(ids, masks[:2], (BF16,) * 2, *operands)
    p4 = parts_call(ids, masks[2:4], (F32, F32), *operands)
    rest = parts_call(ids, masks[4:], (BF16, BF16, F32, F32), *operands)
    totals = []
    for index in range(2):
        passed = flip(p6[index], "fs", 2).astype(F32)
        summed = flip((p4[index] + passed).astype(BF16), "fs", 4)
        near = flip(rest[index], "fs", 2)
        totals.append(settle_call(rest[2 + index], summed, near, (BF16, F32)[index]))
    (given, norm_given), (kept, norm_kept) = totals
    got = flip(given, "fs", 1)
    weight_grad = join_call(ids, kept, got)
    norms = norm_given + norm_kept

    grad_send = product_call(ids, weight_masks, weights, [cot_pair], BF16)
    grad_got = flip(grad_send, "fs", 1)
    grad_mine = product_call(ids, weight_masks, weights, [cot_mine], F32)
    gate_grad, up_grad, edge, head, sums = grads_call(
        ids, up_pre, halo, gate_value, conv_weight, bias, grad_mine, grad_got
    )
    after = shift(head, "fs", -1)
    for tap in range(tap_count - 1):
        lead = tap_count - 1 - tap
        late = conv_weight[tap][None, :] * after[:lead]
        edge = edge + jnp.pad(late, ((EDGE - lead, 0), (0, 0)))
    up_grad = lax.dynamic_update_slice(up_grad, edge.astype(BF16), (tokens - EDGE, 0))

    pack = lax.dynamic_update_slice(sums, norms, (tap_count + 1, 0))
    v0 = pack + flip(pack, "fs", 4)
    values = (v0, *(flip(v0, "fs", mask) for mask in (2, 1, 3)))
    tap_grad, bias_grad, unit_norms = finish_call(ids, values, tap_count)
    return (up_grad, gate_grad, weight_grad, tap_grad, bias_grad[0], unit_norms[0])


def gathered(up_pre, gate_value, out_cotangent, down_weight, conv_weight, conv_bias):
    tap_count = conv_weight.shape[0]
    tokens = up_pre.shape[0]
    before = shift(up_pre[tokens - (tap_count - 1) :], "fs", 1)
    padded = jnp.concatenate([before, up_pre], 0).astype(F32)
    conv_out = jnp.zeros(up_pre.shape, F32) + conv_bias[None, :]
    for tap in range(tap_count):
        conv_out = conv_out + conv_weight[tap][None, :] * padded[tap : tap + tokens]
    sigmoid_val = jax.nn.sigmoid(conv_out)
    activated = conv_out * sigmoid_val
    gate_float = gate_value.astype(F32)
    hidden = (activated * gate_float).astype(BF16)
    full_cot = lax.all_gather(out_cotangent, "tp", axis=1, tiled=True)
    full_weight = lax.all_gather(down_weight, "fs", axis=0, tiled=True)
    hidden_grad = jnp.dot(full_cot, full_weight, preferred_element_type=F32)
    gate_grad = (hidden_grad * activated).astype(BF16)
    conv_grad = hidden_grad * gate_float * sigmoid_val * (1.0 + conv_out * (1.0 - sigmoid_val))
    after = jnp.concatenate([conv_grad, shift(conv_grad[: tap_count - 1], "fs", -1)], 0)
    up_grad = jnp.zeros(up_pre.shape, F32)
    for tap in range(tap_count):
        lead = tap_count - 1 - tap
        up_grad = up_grad + conv_weight[tap][None, :] * after[lead : lead + tokens]
    sums = [jnp.sum(conv_grad * padded[tap : tap + tokens], axis=0) for tap in range(tap_count)]
    sums = lax.psum(jnp.stack(sums + [jnp.sum(conv_grad, axis=0)]), "fs")
    partial_value = jnp.einsum("td,tf->df", full_cot, hidden, preferred_element_type=F32)
    weight_grad = lax.psum_scatter(partial_value, "fs", scatter_dimension=0, tiled=True)
    unit_norms = lax.psum(jnp.sum(weight_grad * weight_grad, axis=0), "fs")
    return (up_grad.astype(BF16), gate_grad, weight_grad, sums[:tap_count], sums[tap_count], unit_norms)


def solution(mesh):
    fs, tp = mesh.shape["fs"], mesh.shape["tp"]
    short = fs == 8 and tp == 4

    def step(*args):
        return (paired if short else gathered)(*args)

    return jax.shard_map(
        step,
        mesh=mesh,
        in_specs=(
            P("fs", "tp"),
            P("fs", "tp"),
            P("fs", "tp"),
            P("fs", "tp"),
            P(None, "tp"),
            P("tp"),
        ),
        out_specs=(P("fs", "tp"), P("fs", "tp"), P("fs", "tp"), P(None, "tp"), P("tp"), P("tp")),
        check_vma=False,
    )
```

```python
import functools

import jax
import jax.numpy as jnp
from jax import lax
from jax.experimental import pallas as pl
from jax.experimental.pallas import tpu as pltpu
from jax.sharding import PartitionSpec as P


GRANT = 20 * 2**20
WIDE = 52 * 2**20
EDGE = 16
BF16, F32 = jnp.bfloat16, jnp.float32


def flip(value, axis, mask):
    count = lax.axis_size(axis)
    return lax.ppermute(value, axis, [(i, i ^ mask) for i in range(count)])


def shift(value, axis, steps):
    count = lax.axis_size(axis)
    initial, last = (max(0, -steps), min(count, count - steps))
    return lax.ppermute(value, axis, [(source, source + steps) for source in range(initial, last)])


def grant(size=GRANT):
    return pltpu.CompilerParams(vmem_limit_bytes=size)


def sigmoid(value):
    return 0.5 * jnp.tanh(0.5 * value) + 0.5


def conv_forward(up_ref, halo_ref, consts_ref, count):
    rows = up_ref.shape[0]
    full = jnp.concatenate([halo_ref[...], up_ref[...]], 0).astype(F32)
    out = consts_ref[count : count + 1, :]
    shifted = []
    for tap in range(count):
        lag = count - 1 - tap
        shifted.append((pltpu.roll(full, lag, 0) if lag else full)[EDGE : EDGE + rows])
        out = out + consts_ref[tap : tap + 1, :] * shifted[tap]
    return shifted, out


def hidden_kernel(ids_ref, up_ref, halo_ref, gate_ref, consts_ref, out_ref, *, count):
    _, out = conv_forward(up_ref, halo_ref, consts_ref, count)
    out_ref[...] = (out * sigmoid(out) * gate_ref[...].astype(F32)).astype(BF16).T


def grads_kernel(
    ids_ref, up_ref, halo_ref, gate_ref, consts_ref, own_ref, got_ref,
    gate_grad_ref, up_grad_ref, edge_ref, head_ref, sums_ref, *, steps, count,
):
    rows = up_ref.shape[0]
    shifted, out = conv_forward(up_ref, halo_ref, consts_ref, count)
    sig = sigmoid(out)
    hidden_grad = jnp.where(pl.program_id(0) < steps, own_ref[...], got_ref[...].astype(F32))
    gate_grad_ref[...] = (hidden_grad * (out * sig)).astype(BF16)
    slope = sig * (1.0 + out * (1.0 - sig))
    grad = hidden_grad * gate_ref[...].astype(F32) * slope
    head_ref[...] = grad[: head_ref.shape[0]]
    width = grad.shape[1]
    padded = jnp.concatenate([grad, jnp.zeros((EDGE, width), F32)], 0)
    total = rows + EDGE
    up_grad = consts_ref[count - 1 : count, :] * grad
    for tap in range(count - 1):
        lead = count - 1 - tap
        up_grad = up_grad + consts_ref[tap : tap + 1, :] * pltpu.roll(padded, total - lead, 0)[:rows]
    up_grad_ref[...] = up_grad.astype(BF16)
    edge_ref[...] = up_grad[rows - EDGE :]
    sums = [jnp.sum(grad * part, 0, keepdims=True) for part in shifted]
    sums.append(jnp.sum(grad, 0, keepdims=True))
    fill = sums_ref.shape[0] - len(sums)
    sums_ref[...] = jnp.concatenate(sums + [jnp.zeros((fill, width), F32)], 0)


COLS = 256


def hidden_call(ids, up_pre, halo, gate, consts, count, mine):
    tokens, units = up_pre.shape
    half = units // 2
    cols = min(COLS, half)
    steps = half // cols

    def spec(rows):
        def at(j, ids_ref):
            y = lax.rem(ids_ref[0], 2)
            return 0, (y if mine else 1 - y) * steps + j

        return pl.BlockSpec((rows, cols), at)

    return pl.pallas_call(
        functools.partial(hidden_kernel, count=count),
        out_shape=jax.ShapeDtypeStruct((half, tokens), BF16),
        grid_spec=pltpu.PrefetchScalarGridSpec(
            num_scalar_prefetch=1,
            grid=(steps,),
            in_specs=[spec(tokens), spec(EDGE), spec(tokens), spec(consts.shape[0])],
            out_specs=pl.BlockSpec((cols, tokens), lambda j, ids_ref: (j, 0)),
        ),
        compiler_params=grant(WIDE),
        cost_estimate=pl.CostEstimate(
            flops=20 * tokens * half, bytes_accessed=6 * tokens * half, transcendentals=0
        ),
    )(ids, up_pre, halo, gate, consts)


def grads_call(ids, up_pre, halo, gate, consts, count, own, got):
    tokens, units = up_pre.shape
    cols = min(COLS, units // 2)
    steps = units // 2 // cols

    def spec(rows):
        def at(j, ids_ref):
            y = lax.rem(ids_ref[0], 2)
            return 0, jnp.where(j < steps, y, 1 - y) * steps + lax.rem(j, steps)

        return pl.BlockSpec((rows, cols), at)

    first = pl.BlockSpec((tokens, cols), lambda j, ids_ref: (0, jnp.minimum(j, steps - 1)))
    second = pl.BlockSpec((tokens, cols), lambda j, ids_ref: (0, jnp.maximum(j - steps, 0)))
    rows = consts.shape[0]
    return pl.pallas_call(
        functools.partial(grads_kernel, steps=steps, count=count),
        out_shape=(
            jax.ShapeDtypeStruct((tokens, units), BF16),
            jax.ShapeDtypeStruct((tokens, units), BF16),
            jax.ShapeDtypeStruct((EDGE, units), F32),
            jax.ShapeDtypeStruct((8, units), F32),
            jax.ShapeDtypeStruct((rows, units), F32),
        ),
        grid_spec=pltpu.PrefetchScalarGridSpec(
            num_scalar_prefetch=1,
            grid=(2 * steps,),
            in_specs=[spec(tokens), spec(EDGE), spec(tokens), spec(rows), first, second],
            out_specs=(spec(tokens), spec(tokens), spec(EDGE), spec(8), spec(rows)),
        ),
        compiler_params=grant(),
        cost_estimate=pl.CostEstimate(
            flops=50 * tokens * units, bytes_accessed=11 * tokens * units, transcendentals=0
        ),
    )(ids, up_pre, halo, gate, consts, own, got)


def parts_kernel(ids_ref, *refs, masks, groups):
    count = sum(len(group) for group in groups)
    hid_mine_ref, hid_pair_ref = refs[count : count + 2]
    out_refs, block_ref = refs[count + 2 : -1], refs[-1]
    rows = block_ref.shape[1]
    per = refs[0].shape[1] // rows
    hidden = jnp.concatenate([hid_mine_ref[...], hid_pair_ref[...]], 1)
    for step, out_ref in enumerate(out_refs):
        block = ids_ref[0] ^ masks[step]
        begin = pl.multiple_of(lax.rem(block, per) * rows, rows)
        for piece in range(len(groups[0])):

            @pl.when(lax.div(block, per) ^ ids_ref[1] == piece)
            def _(piece=piece, begin=begin):
                top = 0
                for group in groups:
                    ref = refs[group[piece]]
                    tokens = ref.shape[0]
                    block_ref[top : top + tokens] = ref[:, pl.ds(begin, rows)]
                    top += tokens

        part = jnp.dot(hidden, block_ref[...], preferred_element_type=F32)
        out_ref[...] = part.astype(out_ref.dtype)


def in_vmem(count):
    return (pl.BlockSpec(memory_space=pltpu.VMEM),) * count


def parts_call(ids, masks, types, rows, cots, hid_mine, hid_pair):
    half, tokens = hid_mine.shape
    count, pieces = len(types), len(cots[0])
    groups = tuple(tuple(range(i * pieces, (i + 1) * pieces)) for i in range(len(cots)))
    return pl.pallas_call(
        functools.partial(parts_kernel, masks=tuple(masks), groups=groups),
        out_shape=tuple(jax.ShapeDtypeStruct((half, rows), kind) for kind in types),
        in_specs=(pl.BlockSpec(memory_space=pltpu.SMEM), *in_vmem(len(cots) * pieces + 2)),
        out_specs=in_vmem(count),
        scratch_shapes=[pltpu.VMEM((2 * tokens, rows), BF16)],
        compiler_params=grant(),
        cost_estimate=pl.CostEstimate(
            flops=4 * tokens * rows * half * count,
            bytes_accessed=4 * tokens * (half + rows * count),
            transcendentals=0,
        ),
    )(ids, *(piece for cot in cots for piece in cot), hid_mine, hid_pair)


def product_kernel(ids_ref, *refs, masks, groups):
    weights, (out_ref, full_ref) = refs[: len(masks)], refs[-2:]
    rows = weights[0].shape[0]
    per = refs[groups[0][0]].shape[1] // rows
    for mask, weight_ref in zip(masks, weights):
        block = ids_ref[0] ^ mask
        at = (lax.div(block, per) ^ ids_ref[1]) * per + lax.rem(block, per)
        full_ref[pl.ds(pl.multiple_of(at * rows, rows), rows), :] = weight_ref[...]
    top = 0
    for group in groups:
        cot = jnp.concatenate([refs[index][...] for index in group], 1)
        part = jnp.dot(cot, full_ref[...], preferred_element_type=F32)
        out_ref[top : top + cot.shape[0]] = part.astype(out_ref.dtype)
        top += cot.shape[0]


def product_call(ids, masks, weights, cots, kind):
    tokens = sum(cot[0].shape[0] for cot in cots)
    rows, half = weights[0].shape
    depth, pieces, start = rows * len(weights), len(cots[0]), len(weights)
    groups = tuple(
        tuple(range(start + i * pieces, start + (i + 1) * pieces)) for i in range(len(cots))
    )
    return pl.pallas_call(
        functools.partial(product_kernel, masks=tuple(masks), groups=groups),
        out_shape=jax.ShapeDtypeStruct((tokens, half), kind),
        in_specs=(
            pl.BlockSpec(memory_space=pltpu.SMEM), *in_vmem(len(weights) + len(cots) * pieces),
        ),
        out_specs=pl.BlockSpec(memory_space=pltpu.VMEM),
        scratch_shapes=[pltpu.VMEM((depth, half), BF16)],
        compiler_params=grant(),
        cost_estimate=pl.CostEstimate(
            flops=2 * tokens * depth * half,
            bytes_accessed=2 * (tokens + half) * depth,
            transcendentals=0,
        ),
    )(ids, *weights, *(piece for cot in cots for piece in cot))


def settle_kernel(own_ref, far_ref, near_ref, out_ref, norm_ref):
    total = own_ref[...] + far_ref[...].astype(F32) + near_ref[...].astype(F32)
    total = total.T
    out_ref[...] = total.astype(out_ref.dtype)
    norm_ref[...] = jnp.sum(total * total, 0, keepdims=True)


def settle_call(own, far, near, kind):
    half, rows = own.shape
    return pl.pallas_call(
        settle_kernel,
        out_shape=(
            jax.ShapeDtypeStruct((rows, half), kind),
            jax.ShapeDtypeStruct((1, half), F32),
        ),
        in_specs=in_vmem(3),
        out_specs=in_vmem(2),
        compiler_params=grant(),
        cost_estimate=pl.CostEstimate(
            flops=6 * half * rows, bytes_accessed=12 * half * rows, transcendentals=0
        ),
    )(own, far, near)


def join_kernel(ids_ref, kept_ref, got_ref, out_ref):
    kept, got = kept_ref[...], got_ref[...].astype(F32)
    first = ids_ref[0] % 2 == 0
    half = kept.shape[1]
    out_ref[:, :half] = jnp.where(first, kept, got)
    out_ref[:, half:] = jnp.where(first, got, kept)


def join_call(ids, kept, got):
    rows, half = kept.shape
    return pl.pallas_call(
        join_kernel,
        out_shape=jax.ShapeDtypeStruct((rows, 2 * half), F32),
        in_specs=(pl.BlockSpec(memory_space=pltpu.SMEM), *in_vmem(2)),
        out_specs=pl.BlockSpec(memory_space=pltpu.VMEM),
        compiler_params=grant(),
        cost_estimate=pl.CostEstimate(
            flops=2 * half * rows, bytes_accessed=14 * half * rows, transcendentals=0
        ),
    )(ids, kept, got)


def finish_kernel(y_ref, v0_ref, v2_ref, v1_ref, v3_ref, tap_ref, bias_ref, norm_ref):
    mine = v0_ref[...] + v2_ref[...]
    pair = v1_ref[...] + v3_ref[...]
    count = tap_ref.shape[0]
    half = norm_ref.shape[1] // 2
    both = mine + pair
    tap_ref[...] = both[:count]
    bias_ref[...] = both[count : count + 1]
    a, b = mine[count + 1 : count + 2, :half], pair[count + 1 : count + 2, :half]
    norm_ref[...] = jnp.where(
        y_ref[0] % 2 == 0, jnp.concatenate([a, b], 1), jnp.concatenate([b, a], 1)
    )


def finish_call(y, values, count):
    units = values[0].shape[1]
    row = jax.ShapeDtypeStruct((1, units), F32)
    return pl.pallas_call(
        finish_kernel,
        out_shape=(jax.ShapeDtypeStruct((count, units), F32), row, row),
        in_specs=[pl.BlockSpec(memory_space=pltpu.SMEM)]
        + [pl.BlockSpec(memory_space=pltpu.VMEM)] * len(values),
        out_specs=(pl.BlockSpec(memory_space=pltpu.VMEM),) * 3,
        compiler_params=grant(),
    )(y, *values)


def paired(up_pre, gate_value, out_cotangent, down_weight, conv_weight, conv_bias):
    tap_count = conv_weight.shape[0]
    tokens, units = up_pre.shape
    half = units // 2
    me, col = lax.axis_index("fs"), lax.axis_index("tp")
    shard = down_weight.shape[0]
    y = me % 2
    ids = lax.optimization_barrier(jnp.stack([me, col]).astype(jnp.int32))
    rows = 8 * ((tap_count + 9) // 8)
    consts = [jnp.pad(conv_weight, ((0, rows - tap_count), (0, 0)))]
    consts += [jnp.pad(conv_bias[None], ((tap_count, rows - tap_count - 1), (0, 0)))]
    consts = consts[0] + consts[1]
    consts = lax.optimization_barrier(consts)

    def features(block):
        over = flip(block, "tp", 2)
        return block, flip(block, "tp", 1), over, flip(over, "tp", 1)

    cot_mine = features(out_cotangent)
    cut = tokens // 2
    cot_pair = []
    for index in range(2):
        piece = lax.slice_in_dim(out_cotangent, index * cut, (index + 1) * cut)
        block = flip(lax.optimization_barrier(piece), "fs", 1)
        cot_pair.append(features(block))

    w_mine = lax.dynamic_slice(down_weight, (0, y * half), (shard, half))
    w_send = lax.dynamic_slice(down_weight, (0, (1 - y) * half), (shard, half))
    weights, weight_masks = [], []
    for block, odd in ((w_mine, 0), (flip(w_send, "fs", 1), 1)):
        far = flip(block, "fs", 4)
        weights += [block, flip(block, "fs", 2), far, flip(far, "fs", 2)]
        weight_masks += [mask ^ odd for mask in (0, 2, 4, 6)]

    halo = shift(up_pre[tokens - EDGE :], "fs", 1)
    forward = (ids, up_pre, halo, gate_value, consts, tap_count)
    hid_send = hidden_call(*forward, False)
    hid_mine = hidden_call(*forward, True)
    hid_pair = flip(hid_send, "fs", 1)

    operands = (shard, (cot_mine, *cot_pair), hid_mine, hid_pair)
    masks = [mask ^ odd for mask in (6, 4, 2, 0) for odd in (1, 0)]
    p6 = parts_call(ids, masks[:2], (BF16,) * 2, *operands)
    p4 = parts_call(ids, masks[2:4], (F32, F32), *operands)
    p2 = parts_call(ids, masks[4:6], (BF16, BF16), *operands)
    p0 = parts_call(ids, masks[6:], (F32, F32), *operands)
    totals = []
    for index in range(2):
        passed = flip(p6[index], "fs", 2).astype(F32)
        summed = flip((p4[index] + passed).astype(BF16), "fs", 4)
        near = flip(p2[index], "fs", 2)
        totals.append(settle_call(p0[index], summed, near, (BF16, F32)[index]))
    (given, norm_given), (kept, norm_kept) = totals
    got = flip(given, "fs", 1)
    weight_grad = join_call(ids, kept, got)
    norms = norm_given + norm_kept

    grad_send = product_call(ids, weight_masks, weights, cot_pair, BF16)
    grad_got = flip(grad_send, "fs", 1)
    grad_mine = product_call(ids, weight_masks, weights, [cot_mine], F32)
    gate_grad, up_grad, edge, head, sums = grads_call(*forward, grad_mine, grad_got)
    after = shift(head, "fs", -1)
    for tap in range(tap_count - 1):
        lead = tap_count - 1 - tap
        late = conv_weight[tap][None, :] * after[:lead]
        edge = edge + jnp.pad(late, ((EDGE - lead, 0), (0, 0)))
    up_grad = lax.dynamic_update_slice(up_grad, edge.astype(BF16), (tokens - EDGE, 0))

    pack = lax.dynamic_update_slice(sums, norms, (tap_count + 1, 0))
    v0 = pack + flip(pack, "fs", 4)
    values = (v0, *(flip(v0, "fs", mask) for mask in (2, 1, 3)))
    tap_grad, bias_grad, unit_norms = finish_call(ids, values, tap_count)
    return (up_grad, gate_grad, weight_grad, tap_grad, bias_grad[0], unit_norms[0])


def gathered(up_pre, gate_value, out_cotangent, down_weight, conv_weight, conv_bias):
    tap_count = conv_weight.shape[0]
    tokens = up_pre.shape[0]
    before = shift(up_pre[tokens - (tap_count - 1) :], "fs", 1)
    padded = jnp.concatenate([before, up_pre], 0).astype(F32)
    conv_out = jnp.zeros(up_pre.shape, F32) + conv_bias[None, :]
    for tap in range(tap_count):
        conv_out = conv_out + conv_weight[tap][None, :] * padded[tap : tap + tokens]
    sigmoid_val = jax.nn.sigmoid(conv_out)
    activated = conv_out * sigmoid_val
    gate_float = gate_value.astype(F32)
    hidden = (activated * gate_float).astype(BF16)
    full_cot = lax.all_gather(out_cotangent, "tp", axis=1, tiled=True)
    full_weight = lax.all_gather(down_weight, "fs", axis=0, tiled=True)
    hidden_grad = jnp.dot(full_cot, full_weight, preferred_element_type=F32)
    gate_grad = (hidden_grad * activated).astype(BF16)
    conv_grad = hidden_grad * gate_float * sigmoid_val * (1.0 + conv_out * (1.0 - sigmoid_val))
    after = jnp.concatenate([conv_grad, shift(conv_grad[: tap_count - 1], "fs", -1)], 0)
    up_grad = jnp.zeros(up_pre.shape, F32)
    for tap in range(tap_count):
        lead = tap_count - 1 - tap
        up_grad = up_grad + conv_weight[tap][None, :] * after[lead : lead + tokens]
    sums = [jnp.sum(conv_grad * padded[tap : tap + tokens], axis=0) for tap in range(tap_count)]
    sums = lax.psum(jnp.stack(sums + [jnp.sum(conv_grad, axis=0)]), "fs")
    partial_value = jnp.einsum("td,tf->df", full_cot, hidden, preferred_element_type=F32)
    weight_grad = lax.psum_scatter(partial_value, "fs", scatter_dimension=0, tiled=True)
    unit_norms = lax.psum(jnp.sum(weight_grad * weight_grad, axis=0), "fs")
    return (up_grad.astype(BF16), gate_grad, weight_grad, sums[:tap_count], sums[tap_count], unit_norms)


def solution(mesh):
    fs, tp = mesh.shape["fs"], mesh.shape["tp"]
    short = fs == 8 and tp == 4

    def step(*args):
        return (paired if short else gathered)(*args)

    return jax.shard_map(
        step,
        mesh=mesh,
        in_specs=(
            P("fs", "tp"),
            P("fs", "tp"),
            P("fs", "tp"),
            P("fs", "tp"),
            P(None, "tp"),
            P("tp"),
        ),
        out_specs=(P("fs", "tp"), P("fs", "tp"), P("fs", "tp"), P(None, "tp"), P("tp"), P("tp")),
        check_vma=False,
    )
```
